512 devices in a mesh: ep: 32 (over z, x), tp: 16 (over y, core).
Axes of the slice: x: 4, y: 8, z: 8, core: 2. Of those that a mesh axis runs over, the one named last changes fastest.
Arguments:
- x_mix: bfloat16 [8192, 2048], P('ep'), may hold values from -6 to 6
- mix_gain: float32 [2048], replicated, may hold values from 0.1 to 1.9
- w_query: bfloat16 [2048, 2048], P(None, 'tp'), may hold values from -0.125 to 0.125
- w_key: bfloat16 [2048, 2048], P(None, 'tp'), may hold values from -0.125 to 0.125
- w_value: bfloat16 [2048, 2048], P(None, 'tp'), may hold values from -0.125 to 0.125
- query_gain: float32 [64], replicated, may hold values from 1 to 1.8
- key_gain: float32 [64], replicated, may hold values from 1 to 1.8
- mix_lambda: float32 [16], P('tp'), may hold values from 0.3 to 0.8
- head_gain: float32 [128], replicated, may hold values from 0.1 to 1.9
- w_mix_out: bfloat16 [2048, 2048], P(None, 'tp'), may hold values from -0.125 to 0.125
- x_exp: bfloat16 [4096, 2048], P('ep'), may hold values from -6 to 6
- exp_gain: float32 [2048], replicated, may hold values from 0.1 to 1.9
- routes: int32 [4096, 4], P('ep'), may hold values from 0 to 31, all different within a row; in each aligned block of 128 rows (0 to 127, 128 to 255, ...) at most 24 rows name the same one
- route_weight: float32 [4096, 4], P('ep'), may hold values from 0.1 to 1
- w_gate: bfloat16 [32, 2048, 2048], P('ep', None, 'tp'), may hold values from -0.375 to 0.375
- w_up: bfloat16 [32, 2048, 2048], P('ep', None, 'tp'), may hold values from -0.375 to 0.375
- w_down: bfloat16 [32, 2048, 2048], P('ep', None, 'tp'), may hold values from -0.03125 to 0.03125
Outputs:
- attn_out: bfloat16 [8192, 2048], P('ep', 'tp')
- moe_out: bfloat16 [4096, 2048], P('ep', 'tp')
The draws below stay inside these ranges and needn't reach their ends.
Inputs may be any that keep to these rules, and one draw needn't show every extreme that they name: `routes`: each row names 4 different experts. In each aligned block of 128 rows (the rows of one index of ep), no expert is named by more than 24 rows, a bound that some block reaches.
All inputs are finite; a program needn't handle non-finite values.
Results may differ from the reference program's by a relative error of at most 0.011.
Values may be sent and summed in bfloat16 or wider, within the bound.
No kernel may reach another device: no remote copies, remote signals or barrier semaphores. Data moves between devices by JAX's collectives and lax.ppermute only.
A program may use at most 128 MiB of HBM per device.

```python
import math
from functools import partial
import jax
import jax.numpy as jnp
import numpy as np
from jax import lax

D = 2048
HEADS = 16
HEAD = 64
FF = 2048
TOPK = 4
TOK_B = 128
TOKENS_A = 8192
TOKENS_B = 4096
EXPERTS = 32
CAP = 24
N_EP = 32


def levels(own_key, shape, pieces, low, high):
    loudness = 1.0
    for dim, parts in pieces:
        steps = jax.random.uniform(jax.random.fold_in(jax.random.fold_in(own_key, 6), dim), (parts,), jnp.float32, low / len(pieces), high / len(pieces))
        loudness = loudness * jnp.repeat(jnp.exp(steps), shape[dim] // parts).reshape((-1,) + (1,) * (len(shape) - 1 - dim))
    return loudness


def assign_block(key, own, number, rows, amount, top, limit, slope):
    ranking = jax.random.permutation(key, amount)
    crowded, ordinary = load_shares(amount, rows * top, limit, slope, True), load_shares(amount, rows * top, limit, slope, False)
    places = jnp.arange(amount)

    def named(tallies, turn):
        used = int((tallies > 0).sum())
        fixed = max(1, used // 4)
        moved = fixed + (places - fixed + turn * (used - fixed)) % max(1, amount - fixed)
        return jnp.zeros((amount,), jnp.int32).at[ranking[jnp.where(places < fixed, places, moved)]].set(jnp.asarray(tallies, jnp.int32))

    tallies = jnp.where(number % 4 == 0, named(crowded, number // 4), named(ordinary, number - number // 4 - 1))
    mixed = jax.random.permutation(jax.random.fold_in(own, 3), amount)
    donor, receiver = mixed[0:amount // 2 * 2:2], mixed[1:amount // 2 * 2:2]
    slack = jnp.minimum(tallies[donor] - 1, limit - tallies[receiver]) // 2
    slack = jnp.where((donor == ranking[0]) | (receiver == ranking[0]) | (tallies[receiver] == 0), 0, jnp.maximum(slack, 0))
    moved = jax.random.randint(jax.random.fold_in(own, 4), (amount // 2,), 0, 1 << 20) % (slack + 1)
    tallies = tallies.at[donor].add(-moved).at[receiver].add(moved)
    labels = jnp.searchsorted(jnp.cumsum(tallies), jnp.arange(rows * top), side="right").astype(jnp.int32)
    listing = labels.reshape(top, rows).T
    listing = listing[jax.random.permutation(jax.random.fold_in(own, 1), rows)]
    turn = jax.random.randint(jax.random.fold_in(own, 2), (rows, 1), 0, top)
    return jnp.take_along_axis(listing, (jnp.arange(top)[None, :] + turn) % top, axis=1)


def load_shares(amount, total, most, lean, full):
    portions = [(1 << 20) // math.isqrt(grade ** lean) + 1 for grade in range(1, amount + 1)]
    largest = most if full else min(most, max(-(-total // amount), total * portions[0] // sum(portions)))
    least = 1 if total - largest >= amount - 1 else 0
    counts, spare = [largest] + [least] * (amount - 1), total - largest - least * (amount - 1)
    while spare > 0:
        candidates = [i for i in range(1, amount) if counts[i] < largest] or [i for i in range(1, amount) if counts[i] < most]
        pool, budget = sum([portions[i] for i in candidates]), spare
        for i in candidates:
            addition = min(most - counts[i], max(1, budget * portions[i] // pool), spare)
            counts[i] = counts[i] + addition
            spare = spare - addition
    return np.array(counts)


def scatter_about(own_key, dims, spread, most, shards=(), kind=jnp.bfloat16):
    values = spread * jax.random.normal(own_key, dims, jnp.float32)
    if shards:
        values = values * levels(own_key, dims, shards, -0.22, 0.18)
    return jnp.clip(values, -most, most).astype(kind)


def setup_inputs(seed: int = 0) -> dict:
    key_of = jax.random.split(jax.random.key(seed), 18)
    x_mix = scatter_about(key_of[0], (TOKENS_A, D), 1.0, 6.0, ((0, 32),))
    mix_gain = jnp.clip(1.0 + 0.18 * jax.random.normal(key_of[1], (D,), jnp.float32), 0.1, 1.9)
    w_query = scatter_about(key_of[2], (D, HEADS * 2 * HEAD), D ** -0.5, 0.125, ((1, 16),))
    w_key = scatter_about(key_of[3], (D, HEADS * 2 * HEAD), D ** -0.5, 0.125, ((1, 16),))
    w_value = scatter_about(key_of[4], (D, HEADS * 2 * HEAD), D ** -0.5, 0.125, ((1, 16),))
    query_gain = jnp.clip(jax.random.uniform(key_of[5], (HEAD,), jnp.float32, 1.0, 1.8), 1.0, 1.8)
    key_gain = jnp.clip(jax.random.uniform(key_of[6], (HEAD,), jnp.float32, 1.0, 1.8), 1.0, 1.8)
    mix_lambda = jnp.clip(0.3 + 0.5 * jax.random.uniform(key_of[7], (HEADS,), jnp.float32) ** levels(key_of[7], (HEADS,), ((0, 16),), -0.2, 0.2), 0.3, 0.8)
    head_gain = jnp.clip(1.0 + 0.18 * jax.random.normal(key_of[8], (2 * HEAD,), jnp.float32), 0.1, 1.9)
    w_mix_out = scatter_about(key_of[9], (HEADS * 2 * HEAD, D), (HEADS * 2 * HEAD) ** -0.5, 0.125, ((1, 16),))
    x_exp = scatter_about(key_of[10], (TOKENS_B, D), 1.0, 6.0, ((0, 32),))
    exp_gain = jnp.clip(1.0 + 0.18 * jax.random.normal(key_of[11], (D,), jnp.float32), 0.1, 1.9)
    routes_keys = jax.random.split(jax.random.fold_in(key_of[12], 1), TOKENS_B // TOK_B)
    routes_turns = jax.random.permutation(jax.random.fold_in(key_of[12], 3), TOKENS_B // TOK_B)
    routes = jax.vmap(lambda own, number: assign_block(jax.random.fold_in(key_of[12], 2), own, number, TOK_B, EXPERTS, TOPK, CAP, 1))(routes_keys, routes_turns).reshape((TOKENS_B, TOPK))
    route_weight = jnp.clip(0.1 + 0.9 * jax.random.uniform(key_of[13], (TOKENS_B, TOPK), jnp.float32) ** levels(key_of[13], (TOKENS_B, TOPK), ((0, 32),), -0.2, 0.2), 0.1, 1.0)
    w_gate = scatter_about(key_of[14], (EXPERTS, D, FF), (D // 9) ** -0.5, 0.375, ((0, 32), (2, 16)))
    w_up = scatter_about(key_of[15], (EXPERTS, D, FF), (D // 9) ** -0.5, 0.375, ((0, 32), (2, 16)))
    w_down = scatter_about(key_of[16], (EXPERTS, FF, D), (FF * 16) ** -0.5, 0.03125, ((0, 32), (2, 16)))
    return dict(x_mix=x_mix, mix_gain=mix_gain, w_query=w_query, w_key=w_key, w_value=w_value, query_gain=query_gain, key_gain=key_gain, mix_lambda=mix_lambda, head_gain=head_gain, w_mix_out=w_mix_out, x_exp=x_exp, exp_gain=exp_gain, routes=routes, route_weight=route_weight, w_gate=w_gate, w_up=w_up, w_down=w_down)


def rms_rows(matrix, gain, epsilon):
    wide = matrix.astype(jnp.float32)
    return wide * lax.rsqrt(lax.optimization_barrier(jnp.mean(wide * wide, axis=-1, keepdims=True)) + epsilon) * gain

def to_float(rounded):
    return lax.optimization_barrier(rounded).astype(jnp.float32)

def slot_ids(chosen_rows, experts, capacity):
    flat_ids = chosen_rows.reshape(-1)
    onehot = (flat_ids[:, None] == jnp.arange(experts, dtype=jnp.int32)[None, :]).astype(jnp.int32)
    before = jnp.cumsum(onehot, axis=0) - onehot
    position = lax.optimization_barrier(jnp.sum(before * onehot, axis=1))
    return flat_ids * capacity + position

def attention_half(x_mix, mix_gain, w_query, w_key, w_value, query_gain, key_gain, mix_lambda, head_gain, w_mix_out):
    seq_len = x_mix.shape[0]
    normed = rms_rows(x_mix, mix_gain, 1e-05).astype(jnp.bfloat16)
    queries = jnp.dot(normed, w_query, preferred_element_type=jnp.float32).reshape(seq_len, HEADS, 2, HEAD)
    queries = (rms_rows(queries, query_gain, 1e-06) * HEAD ** (-0.5)).astype(jnp.bfloat16)
    key_rows = jnp.dot(normed, w_key, preferred_element_type=jnp.float32).reshape(seq_len, HEADS, 2, HEAD)
    key_rows = rms_rows(key_rows, key_gain, 1e-06).astype(jnp.bfloat16)
    values = jnp.dot(normed, w_value, preferred_element_type=jnp.float32).astype(jnp.bfloat16)
    values = values.reshape(seq_len, HEADS, 2 * HEAD)
    position = jnp.arange(seq_len, dtype=jnp.int32)
    visible = position[None, :] <= position[:, None]

    def one_head(operands):
        query_head, key_head, value_head, lambda_head = operands
        scores = jnp.einsum('cqd,ckd->cqk', to_float(query_head), to_float(key_head))
        weights_exp = jnp.where(visible[None], jnp.exp(scores), 0.0)
        denominator = lax.optimization_barrier(jnp.sum(weights_exp, axis=-1))
        numerator = jnp.einsum('cqk,kd->cqd', to_float(weights_exp.astype(jnp.bfloat16)), to_float(value_head))
        head_mix = numerator[0] / denominator[0][:, None] - lambda_head * numerator[1] / denominator[1][:, None]
        return (rms_rows(head_mix, head_gain, 1e-05) * 0.8).astype(jnp.bfloat16)
    outputs = lax.map(one_head, (queries.transpose(1, 2, 0, 3), key_rows.transpose(1, 2, 0, 3), values.transpose(1, 0, 2), mix_lambda))
    head_rows = outputs.transpose(1, 0, 2).reshape(seq_len, HEADS * 2 * HEAD)
    return jnp.dot(head_rows, w_mix_out, preferred_element_type=jnp.float32).astype(jnp.bfloat16)

def place_rows(slot_index, pair_rows):
    return jnp.zeros((EXPERTS * CAP,), jnp.int32).at[slot_index].set(pair_rows)

def mark_slots(slot_index):
    return jnp.zeros((EXPERTS * CAP,), jnp.bool_).at[slot_index].set(True)

def expert_half(x_exp, exp_gain, routes, route_weight, w_gate, w_up, w_down):
    blocks = N_EP
    normed = rms_rows(x_exp, exp_gain, 1e-05).astype(jnp.bfloat16).reshape(blocks, TOK_B, D)
    slot_index = jax.vmap(partial(slot_ids, experts=EXPERTS, capacity=CAP))(routes.reshape(blocks, TOK_B, TOPK))
    pair_rows = jnp.arange(TOK_B * TOPK, dtype=jnp.int32) // TOPK
    source = jax.vmap(partial(place_rows, pair_rows=pair_rows))(slot_index)
    filled = jax.vmap(mark_slots)(slot_index)
    pair_weight = route_weight.reshape(blocks, TOK_B * TOPK)

    def one_expert(running, expert):
        src_rows = lax.dynamic_slice_in_dim(source, expert * CAP, CAP, 1)
        full_slots = lax.dynamic_slice_in_dim(filled, expert * CAP, CAP, 1)
        inputs = jnp.take_along_axis(normed, src_rows[:, :, None], axis=1)
        inputs = jnp.where(full_slots[:, :, None], inputs, jnp.zeros_like(inputs)).reshape(blocks * CAP, D)
        gate_pre = jnp.dot(inputs, w_gate[expert], preferred_element_type=jnp.float32)
        up_pre = jnp.dot(inputs, w_up[expert], preferred_element_type=jnp.float32)
        gate_pre = jnp.minimum(gate_pre, 7.0)
        up_pre = jnp.clip(up_pre, -7.0, 7.0)
        hidden = (gate_pre * jax.nn.sigmoid(1.702 * gate_pre) * (up_pre + 1.0)).astype(jnp.bfloat16)
        result = jnp.dot(hidden, w_down[expert], preferred_element_type=jnp.float32).astype(jnp.bfloat16)
        result = result.reshape(blocks, CAP, D)
        chosen = slot_index // CAP == expert
        place_index = slot_index % CAP
        combine = jnp.where(chosen, pair_weight, 0.0)
        onehot = place_index[:, :, None] == jnp.arange(CAP, dtype=jnp.int32)[None, None, :]
        matrix = jnp.where(onehot, combine[:, :, None], 0.0)
        matrix = lax.optimization_barrier(jnp.sum(matrix.reshape(blocks, TOK_B, TOPK, CAP), axis=2))
        running = running + jnp.einsum('brc,bcd->brd', matrix, to_float(result), precision=lax.Precision.HIGHEST)
        return (running, None)
    start = jnp.zeros((blocks, TOK_B, D), jnp.float32)
    summed, unused = lax.scan(one_expert, start, jnp.arange(EXPERTS, dtype=jnp.int32))
    return summed.reshape(blocks * TOK_B, D).astype(jnp.bfloat16)

def reference(x_mix, mix_gain, w_query, w_key, w_value, query_gain, key_gain, mix_lambda, head_gain, w_mix_out, x_exp, exp_gain, routes, route_weight, w_gate, w_up, w_down):
    attn_out = attention_half(x_mix, mix_gain, w_query, w_key, w_value, query_gain, key_gain, mix_lambda, head_gain, w_mix_out)
    moe_out = expert_half(x_exp, exp_gain, routes, route_weight, w_gate, w_up, w_down)
    return (attn_out, moe_out)
```

```python
import jax
import jax.numpy as jnp
from jax import lax
from jax.experimental import pallas as pl
from jax.experimental.pallas import tpu as pltpu
from jax.sharding import Mesh
from jax.sharding import PartitionSpec as P

BF = jnp.bfloat16
F32 = jnp.float32
EP = ("z", "x")
TP = ("g", "r", "c")
QUAD = ("r", "c")


def dot(a, b, dims=((1,), (0,))):
    return lax.dot_general(a, b, (dims, ((), ())), preferred_element_type=F32)


def call(kernel, shapes, scratch=(), smem_first=True, count=0):
    specs = [pl.BlockSpec(memory_space=pltpu.VMEM)] * count
    if smem_first:
        specs = [pl.BlockSpec(memory_space=pltpu.SMEM)] + specs
    multiple = isinstance(shapes, (list, tuple))
    out_specs = pl.BlockSpec(memory_space=pltpu.VMEM)
    return pl.pallas_call(
        kernel,
        out_shape=tuple(shapes) if multiple else shapes,
        in_specs=specs,
        out_specs=tuple([out_specs] * len(shapes)) if multiple else out_specs,
        scratch_shapes=list(scratch),
    )


def rms(wide, gain, epsilon):
    scale = lax.rsqrt(jnp.mean(wide * wide, axis=-1, keepdims=True) + epsilon)
    return wide * scale * gain


def expert_tables(routes_ref, experts):
    tokens = routes_ref.shape[1]
    expert = lax.broadcasted_iota(jnp.int32, (experts, tokens), 0)
    named = jnp.zeros((experts, tokens), jnp.bool_)
    for k in range(routes_ref.shape[0]):
        named = named | (routes_ref[k : k + 1, :] == expert)
    earlier = lax.broadcasted_iota(jnp.int32, (tokens, tokens), 0) < lax.broadcasted_iota(
        jnp.int32, (tokens, tokens), 1
    )
    counts = dot(
        jnp.where(named, 1.0, 0.0).astype(BF), jnp.where(earlier, 1.0, 0.0).astype(BF)
    )
    return jnp.where(named, counts, -1.0), expert


def spread(table, times):
    rows, lanes = table.shape
    return jnp.broadcast_to(table[:, None, :], (rows, times, lanes)).reshape(rows * times, lanes)


def dispatch_kernel(place_ref, x_ref, gain_ref, routes_ref, out_ref):
    experts = out_ref.shape[0]
    position, _ = expert_tables(routes_ref, experts)
    tokens, width = x_ref.shape
    chunk = width // 4
    wide = spread(position, 24)
    row = lax.broadcasted_iota(jnp.int32, wide.shape, 0) % 24
    wanted = (row % 6 + 6 * place_ref[0]).astype(F32)
    hit = wide == wanted
    normed = rms(x_ref[...].astype(F32), gain_ref[...], 1e-05).astype(BF)
    total = None
    for part in range(4):
        pick = jnp.where(hit & (row // 6 == part), 1.0, 0.0).astype(BF)
        piece = dot(pick, normed[:, part * chunk : (part + 1) * chunk])
        total = piece if total is None else total + piece
    out_ref[...] = total.astype(BF).reshape(out_ref.shape)


def qkv_kernel(x_ref, gain_ref, wq_ref, wk_ref, wv_ref, qg_ref, kg_ref, q_ref, kv_ref):
    normed = rms(x_ref[...].astype(F32), gain_ref[...], 1e-05).astype(BF)

    def component_norm(wide, gain):
        low = lax.broadcasted_iota(jnp.int32, wide.shape, 1) < 64
        square = wide * wide
        first = jnp.sum(jnp.where(low, square, 0.0), axis=-1, keepdims=True)
        second = jnp.sum(jnp.where(low, 0.0, square), axis=-1, keepdims=True)
        scale = jnp.where(
            low, lax.rsqrt(first / 64 + 1e-06), lax.rsqrt(second / 64 + 1e-06)
        )
        return wide * scale * gain

    q = (component_norm(dot(normed, wq_ref[...]), qg_ref[...]) * 0.125).astype(BF)
    k = component_norm(dot(normed, wk_ref[...]), kg_ref[...]).astype(BF)
    v = dot(normed, wv_ref[...]).astype(BF)
    for n in range(q_ref.shape[0]):
        q_ref[n] = q
    for n in range(kv_ref.shape[0]):
        kv_ref[n, :, 0:128] = k
        kv_ref[n, :, 128:256] = v


def flash_kernel(place_ref, q_ref, kv_ref, out_ref, total_ref):
    z = place_ref[0]
    x = place_ref[1]
    groups, rows = q_ref.shape[0], q_ref.shape[1]
    keys = kv_ref.shape[1]
    total_ref[...] = jnp.zeros_like(total_ref)
    ones = jnp.ones((2 * keys, 128), BF)

    def step(pair, masked):
        kv = kv_ref[pl.ds(2 * pair, 2)].reshape(2 * keys, 256)
        value = jnp.concatenate([kv[:, 128:256], ones], axis=1)
        for group in range(groups):
            for comp in range(2):
                lanes = slice(64 * comp, 64 * comp + 64)
                scores = dot(q_ref[group, :, lanes], kv[:, lanes], ((1,), (1,)))
                weight = jnp.exp(scores)
                if masked:
                    col = lax.broadcasted_iota(jnp.int32, scores.shape, 1)
                    block = 2 * pair + col // keys
                    key_pos = 1024 * block + 256 * x + col % keys
                    query_pos = (
                        1024 * z
                        + rows * group
                        + lax.broadcasted_iota(jnp.int32, scores.shape, 0)
                    )
                    weight = jnp.where(key_pos <= query_pos, weight, 0.0)
                total_ref[comp, group] += dot(weight.astype(BF), value)

    def free_step(pair, carry):
        step(pair, False)
        return carry

    lax.fori_loop(0, z // 2, free_step, 0)
    step(z // 2, True)
    lane = lax.broadcasted_iota(jnp.int32, (rows, 128), 1)
    for group in range(groups):
        first = total_ref[0, group, :, 128:256]
        second = total_ref[1, group, :, 128:256]
        first_high = first.astype(BF).astype(F32)
        second_high = second.astype(BF).astype(F32)
        sums = jnp.where(
            lane < 32,
            first_high,
            jnp.where(
                lane < 64,
                first - first_high,
                jnp.where(lane < 96, second_high, second - second_high),
            ),
        )
        out_ref[group, :, 0:128] = total_ref[0, group, :, 0:128].astype(BF)
        out_ref[group, :, 128:256] = total_ref[1, group, :, 0:128].astype(BF)
        out_ref[group, :, 256:384] = sums.astype(BF)


def mix_kernel(lam_ref, part_ref, gain_ref, out_ref):
    total = part_ref[0].astype(F32)
    for n in range(1, part_ref.shape[0]):
        total = total + part_ref[n].astype(F32)
    sums = total[:, 256:384]
    first = sums[:, 0:1] + sums[:, 32:33]
    second = sums[:, 64:65] + sums[:, 96:97]
    mix = total[:, 0:128] / first - lam_ref[0] * total[:, 128:256] / second
    rows = (rms(mix, gain_ref[...], 1e-05) * 0.8).astype(BF)
    half = rows.shape[0] // 2
    for n in range(out_ref.shape[0] // 2):
        out_ref[2 * n] = rows[0:half]
        out_ref[2 * n + 1] = rows[half:]


def project_kernel(rows_ref, own_ref, other_ref, own_out, other_out):
    rows = jnp.concatenate([rows_ref[n] for n in range(rows_ref.shape[0])], axis=1)
    own_out[...] = dot(rows, own_ref[...]).astype(BF)
    other_out[...] = dot(rows, other_ref[...]).astype(BF)


def hidden_kernel(place_ref, in_ref, *refs):
    weights, out_ref = refs[:-1], refs[-1]
    place = place_ref[0]
    sources = in_ref.shape[0]
    flat = in_ref[...].reshape(sources * 24, in_ref.shape[2])
    count = sources * 6
    line = lax.broadcasted_iota(jnp.int32, (count, sources * 24), 0)
    slot = lax.broadcasted_iota(jnp.int32, (count, sources * 24), 1)
    base = (line // 6) * 24 + line % 6
    pieces = []
    for part in range(4):
        pick = jnp.where(slot == base + 6 * part, 1.0, 0.0).astype(BF)
        pieces.append(dot(pick, flat).astype(BF))
    rows = jnp.concatenate(pieces, axis=1)
    for n in range(4):
        gate = jnp.minimum(dot(rows, weights[2 * n][0]), 7.0)
        up = jnp.clip(dot(rows, weights[2 * n + 1][0]), -7.0, 7.0)
        hidden = (gate * jax.nn.sigmoid(1.702 * gate) * (up + 1.0)).astype(BF)
        for peer in range(out_ref.shape[0]):
            out_ref[peer, place ^ n] = hidden


def down_kernel(place_ref, hidden_ref, *refs):
    weights, out_ref = refs[:-1], refs[-1]
    place = place_ref[0]
    rows = jnp.concatenate(
        [hidden_ref[g, a] for g in range(hidden_ref.shape[0]) for a in range(4)], axis=1
    )
    count = rows.shape[0]
    sources = count // 6
    wide = lax.broadcasted_iota(jnp.int32, (sources * 8, count), 0)
    line = lax.broadcasted_iota(jnp.int32, (sources * 8, count), 1)
    hit = ((wide // 8) * 6 + wide % 8 == line) & (wide % 8 < 6)
    pick = jnp.where(hit, 1.0, 0.0).astype(BF)
    for n in range(4):
        result = dot(rows, weights[n][0]).astype(BF)
        result = dot(pick, result).astype(BF)
        out_ref[:, place ^ n] = result.reshape(sources, 8, result.shape[1])


def combine_kernel(routes_ref, weight_ref, rows_ref, out_ref):
    experts = rows_ref.shape[0] // 4
    position, expert = expert_tables(routes_ref, experts)
    weight = jnp.zeros(position.shape, F32)
    for k in range(routes_ref.shape[0]):
        weight = weight + jnp.where(routes_ref[k : k + 1, :] == expert, weight_ref[k : k + 1, :], 0.0)
    wide = spread(position, 32)
    row = lax.broadcasted_iota(jnp.int32, wide.shape, 0) % 32
    slot = jnp.where(row % 8 < 6, (row // 8) * 6 + row % 8, 1000).astype(F32)
    table = jnp.where(wide == slot, spread(weight, 32), 0.0)
    high = table.astype(BF)
    low = (table - high.astype(F32)).astype(BF)
    rows = rows_ref[...].reshape(experts * 32, rows_ref.shape[2])
    dims = ((0,), (0,))
    out_ref[...] = (dot(high, rows, dims) + dot(low, rows, dims)).astype(BF)


def exchange(a, axes):
    return lax.all_to_all(a, axes, 0, 0, tiled=True)


def swap(a, axes, size, flip):
    return lax.ppermute(a, axes, [(n, n ^ flip) for n in range(size)])


def body(
    x_mix,
    mix_gain,
    w_query,
    w_key,
    w_value,
    query_gain,
    key_gain,
    mix_lambda,
    head_gain,
    w_mix_out,
    x_exp,
    exp_gain,
    routes,
    route_weight,
    w_gate,
    w_up,
    w_down,
):
    core = lax.axis_index("c")
    place = (lax.axis_index("r") * 2 + core).astype(jnp.int32)[None]
    where = jnp.stack([lax.axis_index("z"), lax.axis_index("x")]).astype(jnp.int32)
    shape = jax.ShapeDtypeStruct
    rows_a = x_mix.shape[0]
    rows_b = x_exp.shape[0]

    own = jnp.concatenate([w_gate, w_up, w_down], axis=0)
    far = swap(own, "r", 2, 1)
    near = swap(own, "c", 2, 1)
    cross = swap(far, "c", 2, 1)
    other_out = swap(w_mix_out, "c", 2, 1)
    quad = (own, near, far, cross)

    routes_t = routes.T
    outgoing = call(dispatch_kernel, shape((32, 24, 512), BF), count=3)(
        place, x_exp, exp_gain[None], routes_t
    )
    incoming = exchange(outgoing, EP)

    two = lambda gain: jnp.concatenate([gain, gain])[None]
    q_send, kv_send = call(
        qkv_kernel,
        (shape((4, rows_a, 128), BF), shape((8, rows_a, 256), BF)),
        smem_first=False,
        count=7,
    )(x_mix, mix_gain[None], w_query, w_key, w_value, two(query_gain), two(key_gain))
    q_all = exchange(q_send, "x")
    kv_all = exchange(kv_send, "z")

    def weight_specs(names):
        return [pl.BlockSpec((1, 2048, 128), lambda n, m=m: (m, 0, 0)) for _ in range(4) for m in names]

    full = lambda s: pl.BlockSpec(s, lambda n: (0,) * len(s))
    hidden = pl.pallas_call(
        hidden_kernel,
        grid=(1,),
        out_shape=shape((4, 4, 192, 128), BF),
        in_specs=[pl.BlockSpec(memory_space=pltpu.SMEM), full((32, 24, 512))] + weight_specs((0, 1)),
        out_specs=full((4, 4, 192, 128)),
    )(place, incoming, *[w for w in quad for _ in range(2)])
    hidden_all = exchange(hidden, "g")

    partial = call(
        flash_kernel,
        shape((4, rows_a, 384), BF),
        scratch=[pltpu.VMEM((2, 4, rows_a, 256), F32)],
        count=2,
    )(where, q_all, kv_all)
    partial_all = exchange(partial, "x")

    result = pl.pallas_call(
        down_kernel,
        grid=(1,),
        out_shape=shape((32, 4, 8, 128), BF),
        in_specs=[pl.BlockSpec(memory_space=pltpu.SMEM), full((4, 4, 192, 128))] + weight_specs((2,)),
        out_specs=full((32, 4, 8, 128)),
    )(place, hidden_all, *quad)
    returned = exchange(result.reshape(128, 8, 128), EP + QUAD)

    head_send = call(mix_kernel, shape((16, rows_a // 2, 128), BF), count=2)(
        mix_lambda, partial_all, head_gain[None]
    )
    head_all = exchange(head_send, TP)
    mine, theirs = call(
        project_kernel,
        (shape((rows_a // 2, 128), BF), shape((rows_a // 2, 128), BF)),
        smem_first=False,
        count=3,
    )(head_all, w_mix_out, other_out)
    received = swap(theirs, "c", 2, 1)
    attn_out = jnp.where(
        core == 0,
        jnp.concatenate([mine, received], axis=0),
        jnp.concatenate([received, mine], axis=0),
    )

    moe_out = call(combine_kernel, shape((rows_b, 128), BF), smem_first=False, count=3)(
        routes_t, route_weight.T, returned
    )
    return (attn_out, moe_out)


def solution(mesh):
    finer = Mesh(mesh.devices.reshape(8, 4, 4, 2, 2), ("z", "x", "g", "r", "c"))
    placed = (
        P(EP, None),
        P(),
        P(None, TP),
        P(None, TP),
        P(None, TP),
        P(),
        P(),
        P(TP),
        P(),
        P(None, TP),
        P(EP, None),
        P(),
        P(EP, None),
        P(EP, None),
        P(EP, None, TP),
        P(EP, None, TP),
        P(EP, None, TP),
    )
    return jax.shard_map(
        body, mesh=finer, in_specs=placed, out_specs=(P(EP, TP), P(EP, TP)), check_vma=False
    )
```

```python
import jax
import jax.numpy as jnp
from jax import lax
from jax.experimental import pallas as pl
from jax.experimental.pallas import tpu as pltpu
from jax.sharding import Mesh
from jax.sharding import PartitionSpec as P


BF = jnp.bfloat16
F32 = jnp.float32
EP = ("w", "v", "x")
TP = ("g", "r", "c")
QUAD = ("r", "c")


def dot(a, b, dims=((1,), (0,))):
    return lax.dot_general(a, b, (dims, ((), ())), preferred_element_type=F32)


def call(kernel, shapes, scratch=(), smem_first=True, count=0):
    specs = [pl.BlockSpec(memory_space=pltpu.VMEM)] * count
    if smem_first:
        specs = [pl.BlockSpec(memory_space=pltpu.SMEM)] + specs
    multiple = isinstance(shapes, (list, tuple))
    out_specs = pl.BlockSpec(memory_space=pltpu.VMEM)
    return pl.pallas_call(
        kernel,
        out_shape=tuple(shapes) if multiple else shapes,
        in_specs=specs,
        out_specs=tuple([out_specs] * len(shapes)) if multiple else out_specs,
        scratch_shapes=list(scratch),
    )


def corner():
    return lax.axis_index("r") * 2 + lax.axis_index("c")


def rms(wide, gain, epsilon):
    scale = lax.rsqrt(jnp.mean(wide * wide, axis=-1, keepdims=True) + epsilon)
    return wide * scale * gain


def expert_tables(routes_ref, experts):
    tokens = routes_ref.shape[1]
    expert = lax.broadcasted_iota(jnp.int32, (experts, tokens), 0)
    named = jnp.zeros((experts, tokens), jnp.bool_)
    for k in range(routes_ref.shape[0]):
        named = named | (routes_ref[k : k + 1, :] == expert)
    earlier = lax.broadcasted_iota(jnp.int32, (tokens, tokens), 0) < lax.broadcasted_iota(
        jnp.int32, (tokens, tokens), 1
    )
    counts = dot(
        jnp.where(named, 1.0, 0.0).astype(BF), jnp.where(earlier, 1.0, 0.0).astype(BF)
    )
    return jnp.where(named, counts, -1.0), expert


def spread(table, times):
    rows, lanes = table.shape
    return jnp.broadcast_to(table[:, None, :], (rows, times, lanes)).reshape(rows * times, lanes)


def dispatch_kernel(x_ref, gain_ref, routes_ref, out_ref):
    experts = out_ref.shape[0]
    position, _ = expert_tables(routes_ref, experts)
    _, width = x_ref.shape
    chunk = width // 4
    wide = spread(position, 24)
    row = lax.broadcasted_iota(jnp.int32, wide.shape, 0) % 24
    wanted = (row % 6 + 6 * corner()).astype(F32)
    hit = wide == wanted
    normed = rms(x_ref[...].astype(F32), gain_ref[...], 1e-05).astype(BF)
    total = None
    for part in range(4):
        pick = jnp.where(hit & (row // 6 == part), 1.0, 0.0).astype(BF)
        piece = dot(pick, normed[:, part * chunk : (part + 1) * chunk])
        total = piece if total is None else total + piece
    out_ref[...] = total.astype(BF).reshape(out_ref.shape)


def qkv_kernel(x_ref, gain_ref, wq_ref, wk_ref, wv_ref, qg_ref, kg_ref, q_ref, kv_ref):
    normed = rms(x_ref[...].astype(F32), gain_ref[...], 1e-05).astype(BF)

    def component_norm(wide, gain):
        low = lax.broadcasted_iota(jnp.int32, wide.shape, 1) < 64
        square = wide * wide
        first = jnp.sum(jnp.where(low, square, 0.0), axis=-1, keepdims=True)
        second = jnp.sum(jnp.where(low, 0.0, square), axis=-1, keepdims=True)
        scale = jnp.where(
            low, lax.rsqrt(first / 64 + 1e-06), lax.rsqrt(second / 64 + 1e-06)
        )
        return wide * scale * jnp.concatenate([gain, gain], axis=1)

    q = (component_norm(dot(normed, wq_ref[...]), qg_ref[...]) * 0.125).astype(BF)
    k = component_norm(dot(normed, wk_ref[...]), kg_ref[...]).astype(BF)
    v = dot(normed, wv_ref[...]).astype(BF)
    q_ref[...] = q
    kv_ref[:, 0:128] = k
    kv_ref[:, 128:256] = v


def flash_kernel(*refs):
    q_refs, kv_refs, outs, total_ref, q_all = refs[0:4], refs[4:8], refs[8:12], refs[12], refs[13]
    w, v, x = (lax.axis_index(name) for name in EP)
    rows = q_refs[0].shape[0]
    keys = kv_refs[0].shape[0]
    half = keys // 2
    ones = jnp.ones((keys, 128), BF)
    for n in range(4):
        q_all[n] = q_refs[n][...]

    def attend(n, masked):
        for comp in range(2):
            lanes = slice(64 * comp, 64 * comp + 64)
            q = q_all[n, :, lanes]
            total = None
            for turn in range(4):
                kv = kv_refs[turn][...]
                value = jnp.concatenate([kv[:, 128:256], ones], axis=1)
                weight = jnp.exp(dot(q, kv[:, lanes], ((1,), (1,))))
                if masked:
                    source = (x + turn) % 4
                    first = 1024 * v + 256 * source
                    second = 1024 * (1 - v) + 256 * source
                    mine = 1024 * v + 256 * x
                    col = lax.broadcasted_iota(jnp.int32, weight.shape, 1)
                    row = lax.broadcasted_iota(jnp.int32, weight.shape, 0)
                    key_pos = jnp.where(col < half, col + first, col - half + second)
                    weight = jnp.where(key_pos <= row + mine, weight, 0.0)
                piece = dot(weight.astype(BF), value)
                total = piece if total is None else total + piece
            total_ref[n, comp] = total

    attend(0, True)

    def later(n, carry):
        attend(n, False)
        return carry

    lax.fori_loop(1, 4 - w, later, 0)
    for n in range(4):

        @pl.when(n + w < 4)
        def _():
            lines = []
            for comp in range(2):
                outs[n][0:rows, 128 * comp : 128 * comp + 128] = total_ref[n, comp, :, 0:128].astype(BF)
                sums = total_ref[n, comp, :, 128:256].T[0:1]
                high = sums.astype(BF).astype(F32)
                lines += [high, sums - high]
            outs[n][rows:, :] = jnp.concatenate(lines + [jnp.zeros((4, rows), F32)], axis=0).astype(BF)


def mix_kernel(lam_ref, *refs):
    parts, gain_ref, out_ref = refs[0:4], refs[4], refs[5]
    total = parts[0][...].astype(F32)
    for n in range(1, 4):
        total = total + parts[n][...].astype(F32)
    rows = total.shape[1]
    lines = total[rows:, :]
    lines = jnp.concatenate([lines, jnp.zeros((120, rows), F32)], axis=0).T
    first = lines[:, 0:1] + lines[:, 1:2]
    second = lines[:, 2:3] + lines[:, 3:4]
    mix = total[0:rows, 0:128] / first - lam_ref[0] * total[0:rows, 128:256] / second
    rows = (rms(mix, gain_ref[...], 1e-05) * 0.8).astype(BF)
    half = rows.shape[0] // 2
    for n in range(out_ref.shape[0] // 2):
        out_ref[2 * n] = rows[0:half]
        out_ref[2 * n + 1] = rows[half:]


def project_kernel(rows_ref, own_ref, other_ref, out_ref, other_out):
    rows = jnp.concatenate([rows_ref[n] for n in range(rows_ref.shape[0])], axis=1)
    count = rows.shape[0]
    spot = pl.multiple_of(lax.axis_index("c") * count, count)
    out_ref[pl.ds(spot, count), :] = dot(rows, own_ref[...]).astype(BF)
    other_out[...] = dot(rows, other_ref[...]).astype(BF)


def finish_kernel(out_ref, received_ref, done_ref):
    count = received_ref.shape[0]
    core = lax.axis_index("c")
    done_ref[...] = out_ref[...]
    done_ref[pl.ds(pl.multiple_of((1 - core) * count, count), count), :] = received_ref[...]


def hidden_kernel(in_ref, *refs):
    weights, out_ref = refs[:-1], refs[-1]
    place = corner()
    sources = in_ref.shape[0]
    flat = in_ref[...].reshape(sources * 24, in_ref.shape[2])
    count = sources * 6
    line = lax.broadcasted_iota(jnp.int32, (count, sources * 24), 0)
    slot = lax.broadcasted_iota(jnp.int32, (count, sources * 24), 1)
    base = (line // 6) * 24 + line % 6
    pieces = []
    for part in range(4):
        pick = jnp.where(slot == base + 6 * part, 1.0, 0.0).astype(BF)
        pieces.append(dot(pick, flat).astype(BF))
    rows = jnp.concatenate(pieces, axis=1)
    for n in range(4):
        gate = jnp.minimum(dot(rows, weights[2 * n][0]), 7.0)
        up = jnp.clip(dot(rows, weights[2 * n + 1][0]), -7.0, 7.0)
        hidden = (gate * jax.nn.sigmoid(1.702 * gate) * (up + 1.0)).astype(BF)
        for peer in range(out_ref.shape[0]):
            out_ref[peer, place ^ n] = hidden


def down_kernel(hidden_ref, *refs):
    weights, out_ref = refs[:-1], refs[-1]
    place = corner()
    rows = jnp.concatenate(
        [hidden_ref[g, a] for g in range(hidden_ref.shape[0]) for a in range(4)], axis=1
    )
    count = rows.shape[0]
    sources = count // 6
    wide = lax.broadcasted_iota(jnp.int32, (sources * 8, count), 0)
    line = lax.broadcasted_iota(jnp.int32, (sources * 8, count), 1)
    hit = ((wide // 8) * 6 + wide % 8 == line) & (wide % 8 < 6)
    pick = jnp.where(hit, 1.0, 0.0).astype(BF)
    for n in range(4):
        result = dot(rows, weights[n][0]).astype(BF)
        result = dot(pick, result).astype(BF)
        out_ref[:, place ^ n] = result.reshape(sources, 8, result.shape[1])


def combine_kernel(routes_ref, weight_ref, rows_ref, out_ref):
    experts = rows_ref.shape[0] // 4
    position, expert = expert_tables(routes_ref, experts)
    weight = jnp.zeros(position.shape, F32)
    for k in range(routes_ref.shape[0]):
        weight = weight + jnp.where(routes_ref[k : k + 1, :] == expert, weight_ref[k : k + 1, :], 0.0)
    wide = spread(position, 32)
    row = lax.broadcasted_iota(jnp.int32, wide.shape, 0) % 32
    slot = jnp.where(row % 8 < 6, (row // 8) * 6 + row % 8, 1000).astype(F32)
    table = jnp.where(wide == slot, spread(weight, 32), 0.0)
    high = table.astype(BF)
    low = (table - high.astype(F32)).astype(BF)
    rows = rows_ref[...].reshape(experts * 32, rows_ref.shape[2])
    dims = ((0,), (0,))
    out_ref[...] = (dot(high, rows, dims) + dot(low, rows, dims)).astype(BF)


def exchange(a, axes):
    return lax.all_to_all(a, axes, 0, 0, tiled=True)


def swap(a, axes, size, flip):
    return lax.ppermute(a, axes, [(n, n ^ flip) for n in range(size)])


def shift(a, axis, size, step, wrap):
    pairs = [(n, (n + step) % size) for n in range(size) if wrap or 0 <= n + step < size]
    return lax.ppermute(a, axis, pairs)


def body(
    x_mix,
    mix_gain,
    w_query,
    w_key,
    w_value,
    query_gain,
    key_gain,
    mix_lambda,
    head_gain,
    w_mix_out,
    x_exp,
    exp_gain,
    routes,
    route_weight,
    w_gate,
    w_up,
    w_down,
):
    shape = jax.ShapeDtypeStruct
    rows_a = x_mix.shape[0]
    rows_b = x_exp.shape[0]

    own = jnp.concatenate([w_gate, w_up, w_down], axis=0)
    far = swap(own, "r", 2, 1)

    routes_t = routes.T
    outgoing = call(dispatch_kernel, shape((32, 24, 512), BF), smem_first=False, count=3)(
        x_exp, exp_gain[None], routes_t
    )
    incoming = exchange(outgoing, EP)

    q_own, kv_own = call(
        qkv_kernel,
        (shape((rows_a, 128), BF), shape((rows_a, 256), BF)),
        smem_first=False,
        count=7,
    )(x_mix, mix_gain[None], w_query, w_key, w_value, query_gain[None], key_gain[None])
    kv_other = swap(kv_own, "v", 2, 1)
    kv_pair = jnp.concatenate([kv_own, kv_other], axis=0)
    kv_all = [kv_pair] + [shift(kv_pair, "x", 4, -n, True) for n in range(1, 4)]
    q_all = [q_own] + [shift(q_own, "w", 4, -n, False) for n in range(1, 4)]

    near = swap(own, "c", 2, 1)
    cross = swap(far, "c", 2, 1)
    other_out = swap(w_mix_out, "c", 2, 1)
    quad = (own, near, far, cross)

    def weight_specs(names):
        return [pl.BlockSpec((1, 2048, 128), lambda n, m=m: (m, 0, 0)) for _ in range(4) for m in names]

    full = lambda s: pl.BlockSpec(s, lambda n: (0,) * len(s))
    hidden = pl.pallas_call(
        hidden_kernel,
        grid=(1,),
        out_shape=shape((4, 4, 192, 128), BF),
        in_specs=[full((32, 24, 512))] + weight_specs((0, 1)),
        out_specs=full((4, 4, 192, 128)),
    )(incoming, *[w for w in quad for _ in range(2)])
    hidden_all = exchange(hidden, "g")

    partial = call(
        flash_kernel,
        [shape((rows_a + 8, 256), BF)] * 4,
        scratch=[pltpu.VMEM((4, 2, rows_a, 256), F32), pltpu.VMEM((4, rows_a, 128), BF)],
        smem_first=False,
        count=8,
    )(*q_all, *kv_all)
    partial_all = [partial[0]] + [shift(partial[n], "w", 4, n, False) for n in range(1, 4)]

    result = pl.pallas_call(
        down_kernel,
        grid=(1,),
        out_shape=shape((32, 4, 8, 128), BF),
        in_specs=[full((4, 4, 192, 128))] + weight_specs((2,)),
        out_specs=full((32, 4, 8, 128)),
    )(hidden_all, *quad)
    returned = exchange(result.reshape(128, 8, 128), EP + QUAD)

    half = rows_a // 2
    head_send = call(mix_kernel, shape((16, half, 128), BF), count=5)(
        mix_lambda, *partial_all, head_gain[None]
    )
    head_all = exchange(head_send, TP)
    mine, theirs = call(
        project_kernel,
        (shape((rows_a, 128), BF), shape((half, 128), BF)),
        smem_first=False,
        count=3,
    )(head_all, w_mix_out, other_out)
    received = swap(theirs, "c", 2, 1)
    attn_out = call(finish_kernel, shape((rows_a, 128), BF), smem_first=False, count=2)(
        mine, received
    )

    moe_out = call(combine_kernel, shape((rows_b, 128), BF), smem_first=False, count=3)(
        routes_t, route_weight.T, returned
    )
    return (attn_out, moe_out)


def solution(mesh):
    finer = Mesh(mesh.devices.reshape(4, 2, 4, 4, 2, 2), EP + TP)
    placed = (
        P(EP, None),
        P(),
        P(None, TP),
        P(None, TP),
        P(None, TP),
        P(),
        P(),
        P(TP),
        P(),
        P(None, TP),
        P(EP, None),
        P(),
        P(EP, None),
        P(EP, None),
        P(EP, None, TP),
        P(EP, None, TP),
        P(EP, None, TP),
    )

    return jax.shard_map(
        body, mesh=finer, in_specs=placed, out_specs=(P(EP, TP), P(EP, TP)), check_vma=False
    )
```

```python
import jax
import jax.numpy as jnp
from jax import lax
from jax.experimental import pallas as pl
from jax.experimental.pallas import tpu as pltpu
from jax.sharding import Mesh
from jax.sharding import PartitionSpec as P


BF = jnp.bfloat16
F32 = jnp.float32
EP = ("w", "v", "x")
TP = ("g", "r", "c")
QUAD = ("r", "c")


def dot(a, b, dims=((1,), (0,))):
    return lax.dot_general(a, b, (dims, ((), ())), preferred_element_type=F32)


def call(kernel, shapes, scratch=(), smem_first=True, count=0):
    specs = [pl.BlockSpec(memory_space=pltpu.VMEM)] * count
    if smem_first:
        specs = [pl.BlockSpec(memory_space=pltpu.SMEM)] + specs
    multiple = isinstance(shapes, (list, tuple))
    out_specs = pl.BlockSpec(memory_space=pltpu.VMEM)
    return pl.pallas_call(
        kernel,
        out_shape=tuple(shapes) if multiple else shapes,
        in_specs=specs,
        out_specs=tuple([out_specs] * len(shapes)) if multiple else out_specs,
        scratch_shapes=list(scratch),
    )


def corner():
    return lax.axis_index("r") * 2 + lax.axis_index("c")


def rms(wide, gain, epsilon):
    scale = lax.rsqrt(jnp.mean(wide * wide, axis=-1, keepdims=True) + epsilon)
    return wide * scale * gain


def expert_tables(routes_ref, experts):
    tokens = routes_ref.shape[1]
    expert = lax.broadcasted_iota(jnp.int32, (experts, tokens), 0)
    named = jnp.zeros((experts, tokens), jnp.bool_)
    for k in range(routes_ref.shape[0]):
        named = named | (routes_ref[k : k + 1, :] == expert)
    earlier = lax.broadcasted_iota(jnp.int32, (tokens, tokens), 0) < lax.broadcasted_iota(
        jnp.int32, (tokens, tokens), 1
    )
    counts = dot(
        jnp.where(named, 1.0, 0.0).astype(BF), jnp.where(earlier, 1.0, 0.0).astype(BF)
    )
    return jnp.where(named, counts, -1.0), expert


def spread(table, times):
    rows, lanes = table.shape
    return jnp.broadcast_to(table[:, None, :], (rows, times, lanes)).reshape(rows * times, lanes)


def dispatch_kernel(x_ref, gain_ref, routes_ref, out_ref):
    experts = out_ref.shape[0]
    position, _ = expert_tables(routes_ref, experts)
    _, width = x_ref.shape
    chunk = width // 4
    wide = spread(position, 24)
    row = lax.broadcasted_iota(jnp.int32, wide.shape, 0) % 24
    wanted = (row % 6 + 6 * corner()).astype(F32)
    hit = wide == wanted
    normed = rms(x_ref[...].astype(F32), gain_ref[...], 1e-05).astype(BF)
    total = None
    for part in range(4):
        pick = jnp.where(hit & (row // 6 == part), 1.0, 0.0).astype(BF)
        piece = dot(pick, normed[:, part * chunk : (part + 1) * chunk])
        total = piece if total is None else total + piece
    out_ref[...] = total.astype(BF).reshape(out_ref.shape)


def qkv_kernel(x_ref, gain_ref, wq_ref, wk_ref, wv_ref, qg_ref, kg_ref, q_ref, kv_ref):
    normed = rms(x_ref[...].astype(F32), gain_ref[...], 1e-05).astype(BF)

    def component_norm(wide, gain):
        low = lax.broadcasted_iota(jnp.int32, wide.shape, 1) < 64
        square = wide * wide
        first = jnp.sum(jnp.where(low, square, 0.0), axis=-1, keepdims=True)
        second = jnp.sum(jnp.where(low, 0.0, square), axis=-1, keepdims=True)
        scale = jnp.where(
            low, lax.rsqrt(first / 64 + 1e-06), lax.rsqrt(second / 64 + 1e-06)
        )
        return wide * scale * jnp.concatenate([gain, gain], axis=1)

    both = dot(normed, jnp.concatenate([wq_ref[...], wk_ref[...]], axis=1))
    q = (component_norm(both[:, 0:128], qg_ref[...]) * 0.125).astype(BF)
    k = component_norm(both[:, 128:256], kg_ref[...]).astype(BF)
    v = dot(normed, wv_ref[...]).astype(BF)
    q_ref[...] = q
    kv_ref[:, 0:128] = k
    kv_ref[:, 128:256] = v


def flash_kernel(steps, *refs):
    size = len(steps)
    q_refs, kv_refs, outs = refs[:size], refs[size : size + 4], refs[size + 4 : 2 * size + 4]
    total_ref = refs[-1]
    w, v, x = (lax.axis_index(name) for name in EP)
    rows = q_refs[0].shape[0]
    keys = kv_refs[0].shape[0]
    half = keys // 2
    ones = jnp.ones((keys, 128), BF)

    def attend(q_ref, comp, masked):
        lanes = slice(64 * comp, 64 * comp + 64)
        total = None
        for turn in range(4):
            kv = kv_refs[turn][...]
            value = jnp.concatenate([kv[:, 128:256], ones], axis=1)
            scores = dot(q_ref[:, lanes], kv[:, lanes], ((1,), (1,)))
            weight = jnp.exp2(scores * 1.4426950408889634)
            if masked:
                source = (x + turn) % 4
                first = 1024 * v + 256 * source
                second = 1024 * (1 - v) + 256 * source
                mine = 1024 * v + 256 * x
                col = lax.broadcasted_iota(jnp.int32, weight.shape, 1)
                row = lax.broadcasted_iota(jnp.int32, weight.shape, 0)
                key_pos = jnp.where(col < half, col + first, col - half + second)
                weight = jnp.where(key_pos <= row + mine, weight, 0.0)
            piece = dot(weight.astype(BF), value)
            total = piece if total is None else total + piece
        total_ref[comp] = total

    for n, step in enumerate(steps):

        @pl.when(w + step < 4)
        def _():
            lines = []
            for comp in range(2):
                attend(q_refs[n], comp, step == 0)
                outs[n][0:rows, 128 * comp : 128 * comp + 128] = total_ref[comp, :, 0:128].astype(BF)
                sums = total_ref[comp, :, 128:256].T[0:1]
                high = sums.astype(BF).astype(F32)
                lines += [high, sums - high]
            outs[n][rows:, :] = jnp.concatenate(lines + [jnp.zeros((4, rows), F32)], axis=0).astype(BF)


def partial_kernel(steps):
    return lambda *refs: flash_kernel(steps, *refs)


def mix_kernel(lam_ref, *refs):
    parts, gain_ref, out_ref = refs[0:4], refs[4], refs[5]
    total = parts[0][...].astype(F32)
    for n in range(1, 4):
        total = total + parts[n][...].astype(F32)
    rows = total.shape[1]
    lines = total[rows:, :]
    lines = jnp.concatenate([lines, jnp.zeros((120, rows), F32)], axis=0).T
    first = lines[:, 0:1] + lines[:, 1:2]
    second = lines[:, 2:3] + lines[:, 3:4]
    mix = total[0:rows, 0:128] / first - lam_ref[0] * total[0:rows, 128:256] / second
    rows = (rms(mix, gain_ref[...], 1e-05) * 0.8).astype(BF)
    half = rows.shape[0] // 2
    for n in range(out_ref.shape[0] // 2):
        out_ref[2 * n] = rows[0:half]
        out_ref[2 * n + 1] = rows[half:]


def project_kernel(rows_ref, own_ref, other_ref, out_ref, other_out):
    rows = jnp.concatenate([rows_ref[n] for n in range(rows_ref.shape[0])], axis=1)
    count = rows.shape[0]
    spot = pl.multiple_of(lax.axis_index("c") * count, count)
    both = dot(rows, jnp.concatenate([own_ref[...], other_ref[...]], axis=1)).astype(BF)
    out_ref[pl.ds(spot, count), :] = both[:, 0:128]
    other_out[...] = both[:, 128:256]


def finish_kernel(out_ref, received_ref, done_ref):
    count = received_ref.shape[0]
    core = lax.axis_index("c")
    done_ref[...] = out_ref[...]
    done_ref[pl.ds(pl.multiple_of((1 - core) * count, count), count), :] = received_ref[...]


def hidden_kernel(in_ref, *refs):
    weights, out_ref = refs[:-1], refs[-1]
    place = corner()
    sources = in_ref.shape[0]
    flat = in_ref[...].reshape(sources * 24, in_ref.shape[2])
    count = sources * 6
    line = lax.broadcasted_iota(jnp.int32, (count, sources * 24), 0)
    slot = lax.broadcasted_iota(jnp.int32, (count, sources * 24), 1)
    base = (line // 6) * 24 + line % 6
    pieces = []
    for part in range(4):
        pick = jnp.where(slot == base + 6 * part, 1.0, 0.0).astype(BF)
        pieces.append(dot(pick, flat).astype(BF))
    rows = jnp.concatenate(pieces, axis=1)
    for n in range(4):
        both = dot(rows, jnp.concatenate([weights[2 * n][0], weights[2 * n + 1][0]], axis=1))
        gate = jnp.minimum(both[:, 0:128], 7.0)
        up = jnp.clip(both[:, 128:256], -7.0, 7.0)
        hidden = (gate * jax.nn.sigmoid(1.702 * gate) * (up + 1.0)).astype(BF)
        for peer in range(out_ref.shape[0]):
            out_ref[peer, place ^ n] = hidden


def down_kernel(hidden_ref, *refs):
    weights, out_ref = refs[:-1], refs[-1]
    place = corner()
    rows = jnp.concatenate(
        [hidden_ref[g, a] for g in range(hidden_ref.shape[0]) for a in range(4)], axis=1
    )
    count = rows.shape[0]
    sources = count // 6
    wide = lax.broadcasted_iota(jnp.int32, (sources * 8, count), 0)
    line = lax.broadcasted_iota(jnp.int32, (sources * 8, count), 1)
    hit = ((wide // 8) * 6 + wide % 8 == line) & (wide % 8 < 6)
    pick = jnp.where(hit, 1.0, 0.0).astype(BF)
    for pair in range(2):
        wide_weight = jnp.concatenate([weights[2 * pair][0], weights[2 * pair + 1][0]], axis=1)
        result = dot(pick, dot(rows, wide_weight).astype(BF)).astype(BF)
        for n in range(2):
            piece = result[:, 128 * n : 128 * n + 128]
            out_ref[:, place ^ (2 * pair + n)] = piece.reshape(sources, 8, 128)


def combine_kernel(routes_ref, weight_ref, rows_ref, out_ref):
    experts = rows_ref.shape[0] // 4
    position, expert = expert_tables(routes_ref, experts)
    weight = jnp.zeros(position.shape, F32)
    for k in range(routes_ref.shape[0]):
        weight = weight + jnp.where(routes_ref[k : k + 1, :] == expert, weight_ref[k : k + 1, :], 0.0)
    wide = spread(position, 32)
    row = lax.broadcasted_iota(jnp.int32, wide.shape, 0) % 32
    slot = jnp.where(row % 8 < 6, (row // 8) * 6 + row % 8, 1000).astype(F32)
    table = jnp.where(wide == slot, spread(weight, 32), 0.0)
    high = table.astype(BF)
    low = (table - high.astype(F32)).astype(BF)
    rows = rows_ref[...].reshape(experts * 32, rows_ref.shape[2])
    dims = ((0,), (0,))
    out_ref[...] = (dot(high, rows, dims) + dot(low, rows, dims)).astype(BF)


def exchange(a, axes):
    return lax.all_to_all(a, axes, 0, 0, tiled=True)


def swap(a, axes, size, flip):
    return lax.ppermute(a, axes, [(n, n ^ flip) for n in range(size)])


def shift(a, axis, size, step, wrap):
    pairs = [(n, (n + step) % size) for n in range(size) if wrap or 0 <= n + step < size]
    return lax.ppermute(a, axis, pairs)


def body(
    x_mix,
    mix_gain,
    w_query,
    w_key,
    w_value,
    query_gain,
    key_gain,
    mix_lambda,
    head_gain,
    w_mix_out,
    x_exp,
    exp_gain,
    routes,
    route_weight,
    w_gate,
    w_up,
    w_down,
):
    shape = jax.ShapeDtypeStruct
    rows_a = x_mix.shape[0]
    rows_b = x_exp.shape[0]

    own = jnp.concatenate([w_gate, w_up, w_down], axis=0)
    far = swap(own, "r", 2, 1)

    routes_t = routes.T
    outgoing = call(dispatch_kernel, shape((32, 24, 512), BF), smem_first=False, count=3)(
        x_exp, exp_gain[None], routes_t
    )
    incoming = exchange(outgoing, EP)

    q_own, kv_own = call(
        qkv_kernel,
        (shape((rows_a, 128), BF), shape((rows_a, 256), BF)),
        smem_first=False,
        count=7,
    )(x_mix, mix_gain[None], w_query, w_key, w_value, query_gain[None], key_gain[None])
    kv_other = swap(kv_own, "v", 2, 1)
    kv_pair = jnp.concatenate([kv_own, kv_other], axis=0)
    kv_all = [kv_pair] + [shift(kv_pair, "x", 4, -n, True) for n in range(1, 4)]
    q_all = [q_own] + [shift(q_own, "w", 4, -n, False) for n in range(1, 4)]

    near = swap(own, "c", 2, 1)
    cross = swap(far, "c", 2, 1)
    other_out = swap(w_mix_out, "c", 2, 1)
    quad = (own, near, far, cross)

    def weight_specs(names):
        return [pl.BlockSpec((1, 2048, 128), lambda n, m=m: (m, 0, 0)) for _ in range(4) for m in names]

    full = lambda s: pl.BlockSpec(s, lambda n: (0,) * len(s))
    hidden = pl.pallas_call(
        hidden_kernel,
        grid=(1,),
        out_shape=shape((4, 4, 192, 128), BF),
        in_specs=[full((32, 24, 512))] + weight_specs((0, 1)),
        out_specs=full((4, 4, 192, 128)),
    )(incoming, *[w for w in quad for _ in range(2)])
    hidden_all = exchange(hidden, "g")

    partial = [None] * 4
    for steps in GROUPS:
        outs = call(
            partial_kernel(steps),
            [shape((rows_a + 8, 256), BF)] * len(steps),
            scratch=[pltpu.VMEM((2, rows_a, 256), F32)],
            smem_first=False,
            count=len(steps) + 4,
        )(*[q_all[n] for n in steps], *kv_all)
        for n, out in zip(steps, outs):
            partial[n] = out
    partial_all = [partial[0]] + [shift(partial[n], "w", 4, n, False) for n in range(1, 4)]

    result = pl.pallas_call(
        down_kernel,
        grid=(1,),
        out_shape=shape((32, 4, 8, 128), BF),
        in_specs=[full((4, 4, 192, 128))] + weight_specs((2,)),
        out_specs=full((32, 4, 8, 128)),
    )(hidden_all, *quad)
    returned = exchange(result.reshape(128, 8, 128), EP + QUAD)

    half = rows_a // 2
    head_send = call(mix_kernel, shape((16, half, 128), BF), count=5)(
        mix_lambda, *partial_all, head_gain[None]
    )
    head_all = exchange(head_send, TP)
    mine, theirs = call(
        project_kernel,
        (shape((rows_a, 128), BF), shape((half, 128), BF)),
        smem_first=False,
        count=3,
    )(head_all, w_mix_out, other_out)
    received = swap(theirs, "c", 2, 1)
    attn_out = call(finish_kernel, shape((rows_a, 128), BF), smem_first=False, count=2)(
        mine, received
    )

    moe_out = call(combine_kernel, shape((rows_b, 128), BF), smem_first=False, count=3)(
        routes_t, route_weight.T, returned
    )
    return (attn_out, moe_out)


GROUPS = ((3, 2, 1), (0,))


def solution(mesh):
    finer = Mesh(mesh.devices.reshape(4, 2, 4, 4, 2, 2), EP + TP)
    placed = (
        P(EP, None),
        P(),
        P(None, TP),
        P(None, TP),
        P(None, TP),
        P(),
        P(),
        P(TP),
        P(),
        P(None, TP),
        P(EP, None),
        P(),
        P(EP, None),
        P(EP, None),
        P(EP, None, TP),
        P(EP, None, TP),
        P(EP, None, TP),
    )

    return jax.shard_map(
        body, mesh=finer, in_specs=placed, out_specs=(P(EP, TP), P(EP, TP)), check_vma=False
    )
```

```python
import jax
import jax.numpy as jnp
from jax import lax
from jax.experimental import pallas as pl
from jax.experimental.pallas import tpu as pltpu
from jax.sharding import Mesh
from jax.sharding import PartitionSpec as P


BF = jnp.bfloat16
F32 = jnp.float32
EP = ("w", "v", "x")
TP = ("g", "r", "c")
QUAD = ("r", "c")


def dot(a, b, dims=((1,), (0,))):
    return lax.dot_general(a, b, (dims, ((), ())), preferred_element_type=F32)


def call(kernel, shapes, scratch=(), smem_first=True, count=0):
    specs = [pl.BlockSpec(memory_space=pltpu.VMEM)] * count
    if smem_first:
        specs = [pl.BlockSpec(memory_space=pltpu.SMEM)] + specs
    multiple = isinstance(shapes, (list, tuple))
    out_specs = pl.BlockSpec(memory_space=pltpu.VMEM)
    return pl.pallas_call(
        kernel,
        out_shape=tuple(shapes) if multiple else shapes,
        in_specs=specs,
        out_specs=tuple([out_specs] * len(shapes)) if multiple else out_specs,
        scratch_shapes=list(scratch),
    )


def corner():
    return lax.axis_index("r") * 2 + lax.axis_index("c")


def rms(wide, gain, epsilon):
    scale = lax.rsqrt(jnp.mean(wide * wide, axis=-1, keepdims=True) + epsilon)
    return wide * scale * gain


def expert_tables(routes_ref, experts):
    tokens = routes_ref.shape[1]
    expert = lax.broadcasted_iota(jnp.int32, (experts, tokens), 0)
    named = jnp.zeros((experts, tokens), jnp.bool_)
    for k in range(routes_ref.shape[0]):
        named = named | (routes_ref[k : k + 1, :] == expert)
    earlier = lax.broadcasted_iota(jnp.int32, (tokens, tokens), 0) < lax.broadcasted_iota(
        jnp.int32, (tokens, tokens), 1
    )
    counts = dot(
        jnp.where(named, 1.0, 0.0).astype(BF), jnp.where(earlier, 1.0, 0.0).astype(BF)
    )
    return jnp.where(named, counts, -1.0), expert


def spread(table, times):
    rows, lanes = table.shape
    return jnp.broadcast_to(table[:, None, :], (rows, times, lanes)).reshape(rows * times, lanes)


def dispatch_kernel(x_ref, gain_ref, routes_ref, out_ref):
    experts = out_ref.shape[0]
    position, _ = expert_tables(routes_ref, experts)
    _, width = x_ref.shape
    chunk = width // 4
    wide = spread(position, 24)
    row = lax.broadcasted_iota(jnp.int32, wide.shape, 0) % 24
    wanted = (row % 6 + 6 * corner()).astype(F32)
    hit = wide == wanted
    normed = rms(x_ref[...].astype(F32), gain_ref[...], 1e-05).astype(BF)
    picks = [
        jnp.where(hit & (row // 6 == part), 1.0, 0.0).astype(BF) for part in range(4)
    ]
    pieces = [normed[:, part * chunk : (part + 1) * chunk] for part in range(4)]
    total = dot(jnp.concatenate(picks, axis=1), jnp.concatenate(pieces, axis=0))
    out_ref[...] = total.astype(BF).reshape(out_ref.shape)


def qkv_kernel(x_ref, gain_ref, wq_ref, wk_ref, wv_ref, qg_ref, kg_ref, q_ref, kv_ref):
    normed = rms(x_ref[...].astype(F32), gain_ref[...], 1e-05).astype(BF)

    def component_norm(wide, gain):
        low = lax.broadcasted_iota(jnp.int32, wide.shape, 1) < 64
        square = wide * wide
        first = jnp.sum(jnp.where(low, square, 0.0), axis=-1, keepdims=True)
        second = jnp.sum(jnp.where(low, 0.0, square), axis=-1, keepdims=True)
        scale = jnp.where(
            low, lax.rsqrt(first / 64 + 1e-06), lax.rsqrt(second / 64 + 1e-06)
        )
        return wide * scale * jnp.concatenate([gain, gain], axis=1)

    both = dot(normed, jnp.concatenate([wq_ref[...], wk_ref[...]], axis=1))
    q = (component_norm(both[:, 0:128], qg_ref[...]) * 0.125).astype(BF)
    k = component_norm(both[:, 128:256], kg_ref[...]).astype(BF)
    v = dot(normed, wv_ref[...]).astype(BF)
    q_ref[...] = q
    kv_ref[:, 0:128] = k
    kv_ref[:, 128:256] = v


def flash_kernel(steps, *refs):
    size = len(steps)
    q_refs, kv_refs, outs = refs[:size], refs[size : size + 4], refs[size + 4 : 2 * size + 4]
    total_ref = refs[-1]
    w, v, x = (lax.axis_index(name) for name in EP)
    rows = q_refs[0].shape[0]
    keys = kv_refs[0].shape[0]
    half = keys // 2
    ones = jnp.ones((keys, 128), BF)

    def attend(q_ref, comp, masked):
        lanes = slice(64 * comp, 64 * comp + 64)
        total = None
        for turn in range(4):
            kv = kv_refs[turn][...]
            value = jnp.concatenate([kv[:, 128:256], ones], axis=1)
            scores = dot(q_ref[:, lanes], kv[:, lanes], ((1,), (1,)))
            weight = jnp.exp2(scores * 1.4426950408889634)
            if masked:
                source = (x + turn) % 4
                first = 1024 * v + 256 * source
                second = 1024 * (1 - v) + 256 * source
                mine = 1024 * v + 256 * x
                col = lax.broadcasted_iota(jnp.int32, weight.shape, 1)
                row = lax.broadcasted_iota(jnp.int32, weight.shape, 0)
                key_pos = jnp.where(col < half, col + first, col - half + second)
                weight = jnp.where(key_pos <= row + mine, weight, 0.0)
            piece = dot(weight.astype(BF), value)
            total = piece if total is None else total + piece
        total_ref[comp] = total

    for n, step in enumerate(steps):

        @pl.when(w + step < 4)
        def _():
            lines = []
            for comp in range(2):
                attend(q_refs[n], comp, step == 0)
                outs[n][0:rows, 128 * comp : 128 * comp + 128] = total_ref[comp, :, 0:128].astype(BF)
                sums = total_ref[comp, :, 128:256].T[0:1]
                high = sums.astype(BF).astype(F32)
                lines += [high, sums - high]
            outs[n][rows:, :] = jnp.concatenate(lines + [jnp.zeros((4, rows), F32)], axis=0).astype(BF)


def partial_kernel(steps):
    return lambda *refs: flash_kernel(steps, *refs)


def mix_kernel(lam_ref, *refs):
    parts, gain_ref, out_ref = refs[0:4], refs[4], refs[5]
    total = parts[0][...].astype(F32)
    for n in range(1, 4):
        total = total + parts[n][...].astype(F32)
    rows = total.shape[1]
    lines = total[rows:, :]
    lines = jnp.concatenate([lines, jnp.zeros((120, rows), F32)], axis=0).T
    first = lines[:, 0:1] + lines[:, 1:2]
    second = lines[:, 2:3] + lines[:, 3:4]
    mix = total[0:rows, 0:128] / first - lam_ref[0] * total[0:rows, 128:256] / second
    rows = (rms(mix, gain_ref[...], 1e-05) * 0.8).astype(BF)
    half = rows.shape[0] // 2
    for n in range(out_ref.shape[0] // 2):
        out_ref[2 * n] = rows[0:half]
        out_ref[2 * n + 1] = rows[half:]


def project_kernel(rows_ref, own_ref, other_ref, out_ref, other_out):
    rows = jnp.concatenate([rows_ref[n] for n in range(rows_ref.shape[0])], axis=1)
    count = rows.shape[0]
    spot = pl.multiple_of(lax.axis_index("c") * count, count)
    both = dot(rows, jnp.concatenate([own_ref[...], other_ref[...]], axis=1)).astype(BF)
    out_ref[pl.ds(spot, count), :] = both[:, 0:128]
    other_out[...] = both[:, 128:256]


def finish_kernel(out_ref, received_ref, done_ref):
    count = received_ref.shape[0]
    core = lax.axis_index("c")
    done_ref[...] = out_ref[...]
    done_ref[pl.ds(pl.multiple_of((1 - core) * count, count), count), :] = received_ref[...]


def hidden_kernel(in_ref, *refs):
    weights, out_ref = refs[:-1], refs[-1]
    place = corner()
    sources = in_ref.shape[0]
    flat = in_ref[...].reshape(sources * 24, in_ref.shape[2])
    count = sources * 6
    line = lax.broadcasted_iota(jnp.int32, (count, sources * 24), 0)
    slot = lax.broadcasted_iota(jnp.int32, (count, sources * 24), 1)
    base = (line // 6) * 24 + line % 6
    pieces = []
    for part in range(4):
        pick = jnp.where(slot == base + 6 * part, 1.0, 0.0).astype(BF)
        pieces.append(dot(pick, flat).astype(BF))
    rows = jnp.concatenate(pieces, axis=1)
    for n in range(4):
        both = dot(rows, jnp.concatenate([weights[2 * n][0], weights[2 * n + 1][0]], axis=1))
        gate = jnp.minimum(both[:, 0:128], 7.0)
        up = jnp.clip(both[:, 128:256], -7.0, 7.0)
        hidden = (gate * jax.nn.sigmoid(1.702 * gate) * (up + 1.0)).astype(BF)
        for peer in range(out_ref.shape[0]):
            out_ref[peer, place ^ n] = hidden


def down_kernel(hidden_ref, *refs):
    weights, out_ref = refs[:-1], refs[-1]
    place = corner()
    rows = jnp.concatenate(
        [hidden_ref[g, a] for g in range(hidden_ref.shape[0]) for a in range(4)], axis=1
    )
    count = rows.shape[0]
    sources = count // 6
    wide = lax.broadcasted_iota(jnp.int32, (sources * 8, count), 0)
    line = lax.broadcasted_iota(jnp.int32, (sources * 8, count), 1)
    hit = ((wide // 8) * 6 + wide % 8 == line) & (wide % 8 < 6)
    pick = jnp.where(hit, 1.0, 0.0).astype(BF)
    for pair in range(2):
        wide_weight = jnp.concatenate([weights[2 * pair][0], weights[2 * pair + 1][0]], axis=1)
        result = dot(pick, dot(rows, wide_weight).astype(BF)).astype(BF)
        for n in range(2):
            piece = result[:, 128 * n : 128 * n + 128]
            out_ref[:, place ^ (2 * pair + n)] = piece.reshape(sources, 8, 128)


def combine_kernel(routes_ref, weight_ref, rows_ref, out_ref):
    experts = rows_ref.shape[0] // 4
    position, expert = expert_tables(routes_ref, experts)
    weight = jnp.zeros(position.shape, F32)
    for k in range(routes_ref.shape[0]):
        weight = weight + jnp.where(routes_ref[k : k + 1, :] == expert, weight_ref[k : k + 1, :], 0.0)
    wide = spread(position, 32)
    row = lax.broadcasted_iota(jnp.int32, wide.shape, 0) % 32
    slot = jnp.where(row % 8 < 6, (row // 8) * 6 + row % 8, 1000).astype(F32)
    table = jnp.where(wide == slot, spread(weight, 32), 0.0)
    high = table.astype(BF)
    low = (table - high.astype(F32)).astype(BF)
    rows = rows_ref[...].reshape(experts * 32, rows_ref.shape[2])
    dims = ((0,), (0,))
    out_ref[...] = (dot(high, rows, dims) + dot(low, rows, dims)).astype(BF)


def exchange(a, axes):
    return lax.all_to_all(a, axes, 0, 0, tiled=True)


def swap(a, axes, size, flip):
    return lax.ppermute(a, axes, [(n, n ^ flip) for n in range(size)])


def shift(a, axis, size, step, wrap):
    pairs = [(n, (n + step) % size) for n in range(size) if wrap or 0 <= n + step < size]
    return lax.ppermute(a, axis, pairs)


def body(
    x_mix,
    mix_gain,
    w_query,
    w_key,
    w_value,
    query_gain,
    key_gain,
    mix_lambda,
    head_gain,
    w_mix_out,
    x_exp,
    exp_gain,
    routes,
    route_weight,
    w_gate,
    w_up,
    w_down,
):
    shape = jax.ShapeDtypeStruct
    rows_a = x_mix.shape[0]
    rows_b = x_exp.shape[0]

    own = jnp.concatenate([w_gate, w_up, w_down], axis=0)
    far = swap(own, "r", 2, 1)

    routes_t = routes.T
    outgoing = call(dispatch_kernel, shape((32, 24, 512), BF), smem_first=False, count=3)(
        x_exp, exp_gain[None], routes_t
    )
    incoming = exchange(outgoing, EP)

    q_own, kv_own = call(
        qkv_kernel,
        (shape((rows_a, 128), BF), shape((rows_a, 256), BF)),
        smem_first=False,
        count=7,
    )(x_mix, mix_gain[None], w_query, w_key, w_value, query_gain[None], key_gain[None])
    kv_other = swap(kv_own, "v", 2, 1)
    kv_pair = jnp.concatenate([kv_own, kv_other], axis=0)
    kv_all = [kv_pair] + [shift(kv_pair, "x", 4, -n, True) for n in range(1, 4)]
    q_all = [q_own] + [shift(q_own, "w", 4, -n, False) for n in range(1, 4)]

    near = swap(own, "c", 2, 1)
    cross = swap(far, "c", 2, 1)
    other_out = swap(w_mix_out, "c", 2, 1)
    quad = (own, near, far, cross)

    def weight_specs(names):
        return [pl.BlockSpec((1, 2048, 128), lambda n, m=m: (m, 0, 0)) for _ in range(4) for m in names]

    full = lambda s: pl.BlockSpec(s, lambda n: (0,) * len(s))
    hidden = pl.pallas_call(
        hidden_kernel,
        grid=(1,),
        out_shape=shape((4, 4, 192, 128), BF),
        in_specs=[full((32, 24, 512))] + weight_specs((0, 1)),
        out_specs=full((4, 4, 192, 128)),
    )(incoming, *[w for w in quad for _ in range(2)])
    hidden_all = exchange(hidden, "g")

    partial = [None] * 4
    for steps in GROUPS:
        outs = call(
            partial_kernel(steps),
            [shape((rows_a + 8, 256), BF)] * len(steps),
            scratch=[pltpu.VMEM((2, rows_a, 256), F32)],
            smem_first=False,
            count=len(steps) + 4,
        )(*[q_all[n] for n in steps], *kv_all)
        for n, out in zip(steps, outs):
            partial[n] = out
    partial_all = [partial[0]] + [shift(partial[n], "w", 4, n, False) for n in range(1, 4)]

    result = pl.pallas_call(
        down_kernel,
        grid=(1,),
        out_shape=shape((32, 4, 8, 128), BF),
        in_specs=[full((4, 4, 192, 128))] + weight_specs((2,)),
        out_specs=full((32, 4, 8, 128)),
    )(hidden_all, *quad)
    returned = exchange(result.reshape(128, 8, 128), EP + QUAD)

    half = rows_a // 2
    head_send = call(mix_kernel, shape((16, half, 128), BF), count=5)(
        mix_lambda, *partial_all, head_gain[None]
    )
    head_all = exchange(head_send, TP)
    mine, theirs = call(
        project_kernel,
        (shape((rows_a, 128), BF), shape((half, 128), BF)),
        smem_first=False,
        count=3,
    )(head_all, w_mix_out, other_out)
    received = swap(theirs, "c", 2, 1)
    attn_out = call(finish_kernel, shape((rows_a, 128), BF), smem_first=False, count=2)(
        mine, received
    )

    moe_out = call(combine_kernel, shape((rows_b, 128), BF), smem_first=False, count=3)(
        routes_t, route_weight.T, returned
    )
    return (attn_out, moe_out)


GROUPS = ((3, 2, 1), (0,))


def solution(mesh):
    finer = Mesh(mesh.devices.reshape(4, 2, 4, 4, 2, 2), EP + TP)
    placed = (
        P(EP, None),
        P(),
        P(None, TP),
        P(None, TP),
        P(None, TP),
        P(),
        P(),
        P(TP),
        P(),
        P(None, TP),
        P(EP, None),
        P(),
        P(EP, None),
        P(EP, None),
        P(EP, None, TP),
        P(EP, None, TP),
        P(EP, None, TP),
    )

    return jax.shard_map(
        body, mesh=finer, in_specs=placed, out_specs=(P(EP, TP), P(EP, TP)), check_vma=False
    )
```
